32 devices in a mesh: ra: 8 (over z, x), cb: 4 (over y, core).
Axes of the slice: x: 2, y: 2, z: 4, core: 2. Of those that a mesh axis runs over, the one named last changes fastest.
Arguments:
- tokens: bfloat16 [64, 1024], P(None, 'ra'), may hold values from -14 to 14, as said below
- norm_gain_a: float32 [1024], P('ra'), may hold values from 0.1 to 1.9
- gate_weight_a: float32 [1024, 2816], P('ra', 'cb'), may hold values from -0.1875 to 0.1875
- up_weight_a: float32 [1024, 2816], P('ra', 'cb'), may hold values from -0.1875 to 0.1875
- down_weight_a: float32 [2816, 1024], P('cb', 'ra'), may hold values from -0.109375 to 0.109375
- norm_gain_b: float32 [1024], P('ra'), may hold values from 0.1 to 1.9
- gate_weight_b: float32 [1024, 2816], P('ra', 'cb'), may hold values from -0.1875 to 0.1875
- up_weight_b: float32 [1024, 2816], P('ra', 'cb'), may hold values from -0.1875 to 0.1875
- down_weight_b: float32 [2816, 1024], P('cb', 'ra'), may hold values from -0.109375 to 0.109375
Outputs:
- stream_out: bfloat16 [64, 1024], P(None, 'ra')
The draws below stay inside these ranges and needn't reach their ends.
Inputs may be any that keep to these rules, and one draw needn't show every extreme that they name: Each feature of tokens carries its own scale, between about 0.3 and 3.3 across features; entries lie within -14 to 14.
All inputs are finite; a program needn't handle non-finite values.
Results may differ from the reference program's by a relative error of at most 0.008.
Values may be sent and summed in bfloat16 or wider, within the bound.
A program may use at most 64 MiB of HBM per device.

```python
import jax
import jax.numpy as jnp
from jax import lax

D = 1024
FF = 2816
TOKENS = 64


def draw_tokens(key, part):
    first_key, second_key = jax.random.split(jax.random.fold_in(key, 17))
    base = jnp.clip(jax.random.normal(first_key, (TOKENS, D), jnp.float32), -4.0, 4.0)
    column_scale = jnp.exp(jax.random.uniform(second_key, (D,), jnp.float32, -1.2, 1.2))
    return (base * column_scale).astype(jnp.bfloat16)


def steps_of(stream_key, shape, cuts, low, largest):
    def one(position, blocks):
        steps = jax.random.uniform(jax.random.fold_in(jax.random.fold_in(stream_key, 6), position), (blocks,), jnp.float32, low / len(cuts), largest / len(cuts))
        return jnp.repeat(jnp.exp(steps), shape[position] // blocks).reshape((-1,) + (1,) * (len(shape) - position - 1))

    loudness = one(*cuts[0])
    for cut in cuts[1:]:
        loudness = loudness * one(*cut)
    return loudness


def gaussian(key, extent, scale, most, shards=(), dtype=jnp.bfloat16):
    level = steps_of(key, extent, shards, -0.22, 0.18) if shards else 1.0
    result = jax.random.normal(key, extent, jnp.float32) * scale * level
    return jnp.minimum(jnp.maximum(result, -most), most).astype(dtype)


def setup_inputs(seed: int = 0) -> dict:
    splits = jax.random.split(jax.random.key(seed), 10)
    return {
        "tokens": draw_tokens(jax.random.fold_in(splits[9], 71), 0),
        "norm_gain_a": jnp.clip(1.0 + 0.18 * jax.random.normal(splits[1], (D,), jnp.float32), 0.1, 1.9),
        "gate_weight_a": gaussian(splits[2], (D, FF), D ** -0.5, 0.1875, ((0, 8), (1, 4)), jnp.float32),
        "up_weight_a": gaussian(splits[3], (D, FF), D ** -0.5, 0.1875, ((0, 8), (1, 4)), jnp.float32),
        "down_weight_a": gaussian(splits[4], (FF, D), FF ** -0.5, 0.109375, ((0, 4), (1, 8)), jnp.float32),
        "norm_gain_b": jnp.clip(1.0 + 0.18 * jax.random.normal(splits[5], (D,), jnp.float32), 0.1, 1.9),
        "gate_weight_b": gaussian(splits[6], (D, FF), D ** -0.5, 0.1875, ((0, 8), (1, 4)), jnp.float32),
        "up_weight_b": gaussian(splits[7], (D, FF), D ** -0.5, 0.1875, ((0, 8), (1, 4)), jnp.float32),
        "down_weight_b": gaussian(splits[8], (FF, D), FF ** -0.5, 0.109375, ((0, 4), (1, 8)), jnp.float32),
    }


residual_weight = 0.5
epsilon = 1e-06

def sublayer(stream, gain, gate_weight, up_weight, down_weight):
    as_float = stream.astype(jnp.float32)
    mean_square = lax.optimization_barrier(jnp.mean(as_float * as_float, axis=1, keepdims=True))
    normed = (as_float * lax.rsqrt(mean_square + epsilon) * gain).astype(jnp.bfloat16)
    gate_sum = jnp.dot(normed, gate_weight.astype(jnp.bfloat16), preferred_element_type=jnp.float32)
    up_sum = jnp.dot(normed, up_weight.astype(jnp.bfloat16), preferred_element_type=jnp.float32)
    hidden = (jax.nn.silu(gate_sum) * up_sum).astype(jnp.bfloat16)
    branch = jnp.dot(hidden, down_weight.astype(jnp.bfloat16), preferred_element_type=jnp.float32)
    return (residual_weight * as_float + branch).astype(jnp.bfloat16)

def reference(tokens, norm_gain_a, gate_weight_a, up_weight_a, down_weight_a, norm_gain_b, gate_weight_b, up_weight_b, down_weight_b):
    middle = sublayer(tokens, norm_gain_a, gate_weight_a, up_weight_a, down_weight_a)
    return sublayer(middle, norm_gain_b, gate_weight_b, up_weight_b, down_weight_b)
```

```python
import functools

import jax
import jax.numpy as jnp
from jax import lax
from jax.experimental import pallas as pl
from jax.experimental.pallas import tpu as pltpu
from jax.sharding import PartitionSpec as P

residual_weight = 0.5
epsilon = 1e-06
MESH = pl.DeviceIdType.MESH
F32, BF16 = jnp.float32, jnp.bfloat16


def dot_t(a, b):
    return lax.dot_general(a, b, (((1,), (1,)), ((), ())), preferred_element_type=F32)


def kernel(
    n, m, x_ref, gain_a, gain_b, wg_a, wu_a, wd_a, wg_b, wu_b, wd_b, out_ref,
    wg_f, wu_f, wd_f, wg_h, wu_h, wd_h, part, slab, hslab, bslab,
    load_sem, part_send, part_recv, hid_send, hid_recv, br_send, br_recv,
):
    me = lax.axis_index("ra")
    mc = lax.axis_index("cb")
    tokens, d = x_ref.shape
    f = wg_a.shape[0]
    t = tokens // n
    width = part.shape[-1]

    barrier = pltpu.get_barrier_semaphore()
    for k in range(1, n):
        pl.semaphore_signal(
            barrier, inc=1, device_id={"ra": lax.rem(me + k, n)}, device_id_type=MESH
        )
    for k in range(1, m):
        pl.semaphore_signal(
            barrier, inc=1, device_id={"cb": lax.rem(mc + k, m)}, device_id_type=MESH
        )

    loads = {}
    for s, (g, u, w) in enumerate(((wg_a, wu_a, wd_a), (wg_b, wu_b, wd_b))):
        for j, (src, dst) in enumerate(((g, wg_f), (u, wu_f), (w, wd_f))):
            loads[s, j] = pltpu.make_async_copy(src, dst.at[s], load_sem.at[s, j])
            loads[s, j].start()

    def cast(s, j):
        src, dst = ((wg_f, wg_h), (wu_f, wu_h), (wd_f, wd_h))[j]
        loads[s, j].wait()
        dst[s] = src[s].astype(BF16)

    def part_copy(s, k):
        peer = lax.rem(me + k, n)
        return pltpu.make_async_remote_copy(
            src_ref=part.at[s, peer], dst_ref=slab.at[s, me],
            send_sem=part_send.at[s, k], recv_sem=part_recv.at[s, me],
            device_id={"ra": peer}, device_id_type=MESH,
        )

    def part_arrival(s, i):
        return pltpu.make_async_remote_copy(
            src_ref=part.at[s, i], dst_ref=slab.at[s, i],
            send_sem=part_send.at[s, 0], recv_sem=part_recv.at[s, i],
            device_id={"ra": i}, device_id_type=MESH,
        )

    def hid_copy(s, k):
        peer = lax.rem(me + k, n)
        return pltpu.make_async_remote_copy(
            src_ref=hslab.at[s, me], dst_ref=hslab.at[s, me],
            send_sem=hid_send.at[s, k], recv_sem=hid_recv.at[s, me],
            device_id={"ra": peer}, device_id_type=MESH,
        )

    def hid_arrival(s, i):
        return pltpu.make_async_remote_copy(
            src_ref=hslab.at[s, i], dst_ref=hslab.at[s, i],
            send_sem=hid_send.at[s, 0], recv_sem=hid_recv.at[s, i],
            device_id={"ra": i}, device_id_type=MESH,
        )

    def br_copy(s, k):
        peer = lax.rem(mc + k, m)
        return pltpu.make_async_remote_copy(
            src_ref=bslab.at[s, mc], dst_ref=bslab.at[s, mc],
            send_sem=br_send.at[s, k], recv_sem=br_recv.at[s, mc],
            device_id={"cb": peer}, device_id_type=MESH,
        )

    def br_arrival(s, i):
        return pltpu.make_async_remote_copy(
            src_ref=bslab.at[s, i], dst_ref=bslab.at[s, i],
            send_sem=br_send.at[s, 0], recv_sem=br_recv.at[s, i],
            device_id={"cb": i}, device_id_type=MESH,
        )

    def sublayer(s, v, gain_ref):
        square = jnp.sum(v * v, axis=1, keepdims=True)
        high = square.astype(BF16).astype(F32)
        low = square - high
        scaled = (v * gain_ref[...]).astype(BF16)
        if s == 0:
            cast(0, 0)
        gate = dot_t(scaled, wg_h[s])
        if s == 0:
            cast(0, 1)
        up = dot_t(scaled, wu_h[s])
        for j in range(n):
            rows = slice(j * t, (j + 1) * t)
            part[s, j, :, :f] = jnp.concatenate([gate[rows], up[rows]], axis=0).astype(BF16)
            part[s, j, :, f:] = jnp.broadcast_to(
                jnp.concatenate([high[rows], low[rows]], axis=0), (2 * t, width - f)
            ).astype(BF16)
        if s == 0:
            pl.semaphore_wait(barrier, n - 1 + m - 1)
        for k in range(1, n):
            part_copy(s, k).start()
        cast(s, 2)
        if s == 0:
            cast(1, 0)
            cast(1, 1)
        total = part[s, me].astype(F32)
        for k in range(1, n):
            i = lax.rem(me + k, n)
            part_arrival(s, i).wait_recv()
            total = total + slab[s, i].astype(F32)
        square_total = total[:t, f : f + 1] + total[t:, f : f + 1]
        row_scale = lax.rsqrt(square_total / (d * n) + epsilon)
        gate_sum = total[:t, :f] * row_scale
        up_sum = total[t:, :f] * row_scale
        hslab[s, me] = (gate_sum / (1.0 + jnp.exp(-gate_sum)) * up_sum).astype(BF16)
        for k in range(1, n):
            hid_copy(s, k).start()
        for k in range(1, n):
            hid_arrival(s, lax.rem(me + k, n)).wait_recv()
        hidden = jnp.concatenate([hslab[s, i].astype(F32) for i in range(n)], axis=0).astype(BF16)
        branch_part = jnp.dot(hidden, wd_h[s], preferred_element_type=F32)
        bslab[s, mc] = branch_part.astype(BF16)
        for k in range(1, m):
            br_copy(s, k).start()
        for k in range(1, m):
            br_arrival(s, lax.rem(mc + k, m)).wait_recv()
        branch = bslab[s, 0].astype(F32)
        for i in range(1, m):
            branch = branch + bslab[s, i].astype(F32)
        return (residual_weight * v + branch).astype(BF16)

    middle = sublayer(0, x_ref[...].astype(F32), gain_a)
    out_ref[...] = sublayer(1, middle.astype(F32), gain_b)

    for s in range(2):
        for k in range(1, n):
            part_copy(s, k).wait_send()
            hid_copy(s, k).wait_send()
        for k in range(1, m):
            br_copy(s, k).wait_send()


def solution(mesh):
    n, m = mesh.shape["ra"], mesh.shape["cb"]

    def per_device(tokens, ga, wg_a, wu_a, wd_a, gb, wg_b, wu_b, wd_b):
        rows, d = tokens.shape
        f = wg_a.shape[1]
        t = rows // n
        width = (f // 128 + 1) * 128
        vmem = pl.BlockSpec(memory_space=pltpu.VMEM)
        hbm = pl.BlockSpec(memory_space=pltpu.HBM)
        dma = pltpu.SemaphoreType.DMA
        return pl.pallas_call(
            functools.partial(kernel, n, m),
            out_shape=jax.ShapeDtypeStruct((rows, d), BF16),
            in_specs=[vmem] * 3 + [hbm] * 6,
            out_specs=vmem,
            scratch_shapes=[
                pltpu.VMEM((2, f, d), F32),
                pltpu.VMEM((2, f, d), F32),
                pltpu.VMEM((2, f, d), F32),
                pltpu.VMEM((2, f, d), BF16),
                pltpu.VMEM((2, f, d), BF16),
                pltpu.VMEM((2, f, d), BF16),
                pltpu.VMEM((2, n, 2 * t, width), BF16),
                pltpu.VMEM((2, n, 2 * t, width), BF16),
                pltpu.VMEM((2, n, t, f), BF16),
                pltpu.VMEM((2, m, rows, d), BF16),
                dma((2, 3)),
                dma((2, n)), dma((2, n)), dma((2, n)), dma((2, n)), dma((2, m)), dma((2, m)),
            ],
            compiler_params=pltpu.CompilerParams(collective_id=0, has_side_effects=True),
        )(tokens, ga.reshape(1, d), gb.reshape(1, d), wg_a.T, wu_a.T, wd_a, wg_b.T, wu_b.T, wd_b)

    weights = (P("ra", "cb"), P("ra", "cb"), P("cb", "ra"))
    placed = (P(None, "ra"), P("ra")) + weights + (P("ra"),) + weights
    return jax.shard_map(
        per_device, mesh=mesh, in_specs=placed, out_specs=P(None, "ra"), check_vma=False
    )
```

```python
import functools

import jax
import jax.numpy as jnp
from jax import lax
from jax.experimental import pallas as pl
from jax.experimental.pallas import tpu as pltpu
from jax.sharding import PartitionSpec as P

residual_weight = 0.5
epsilon = 1e-06
CHAINS = 1
MESH = pl.DeviceIdType.MESH
F32, BF16 = jnp.float32, jnp.bfloat16


def dot_t(a, b):
    return lax.dot_general(a, b, (((1,), (1,)), ((), ())), preferred_element_type=F32)


def partner(me, k, n):
    if n & (n - 1):
        return lax.rem(me + k, n)
    peer, bit = me, 1
    while bit < n:
        if k & bit:
            peer = peer + bit - 2 * bit * ((me // bit) % 2)
        bit *= 2
    return peer


def giver(me, k, n):
    return lax.rem(me + n - k, n) if n & (n - 1) else partner(me, k, n)


def kernel(
    n, m, chains, x_in, gain_a, gain_b, wg_a, wu_a, wd_a, wg_b, wu_b, wd_b, out_ref,
    x_ref, gains, wg_f, wu_f, wd_f, wg_h, wu_h, wd_h, part, slab, hslab, bslab,
    load_sem, small_sem, part_send, part_recv, hid_send, hid_recv, br_send, br_recv,
):
    me = lax.axis_index("ra")
    mc = lax.axis_index("cb")
    tokens, d = x_in.shape
    f = wg_a.shape[0]
    rows = tokens // chains
    t = rows // n
    width = part.shape[-1]
    far = range(n - 1, 0, -1)
    wide = range(m - 1, 0, -1)

    barrier = pltpu.get_barrier_semaphore()
    for k in far:
        pl.semaphore_signal(
            barrier, inc=1, device_id={"ra": partner(me, k, n)}, device_id_type=MESH
        )
    for k in wide:
        pl.semaphore_signal(
            barrier, inc=1, device_id={"cb": partner(mc, k, m)}, device_id_type=MESH
        )

    small = [
        pltpu.make_async_copy(x_in, x_ref, small_sem.at[0]),
        pltpu.make_async_copy(gain_a, gains.at[0], small_sem.at[1]),
        pltpu.make_async_copy(gain_b, gains.at[1], small_sem.at[2]),
    ]
    for copy in small:
        copy.start()
    loads = {}
    for s, (g, u, w) in enumerate(((wg_a, wu_a, wd_a), (wg_b, wu_b, wd_b))):
        for j, (src, dst) in enumerate(((g, wg_f), (u, wu_f), (w, wd_f))):
            loads[s, j] = pltpu.make_async_copy(src, dst.at[s], load_sem.at[s, j])
            loads[s, j].start()

    def cast(s, j):
        src, dst = ((wg_f, wg_h), (wu_f, wu_h), (wd_f, wd_h))[j]
        loads[s, j].wait()
        dst[s] = src[s].astype(BF16)

    def remote(src, dst, send, recv, axis, peer):
        return pltpu.make_async_remote_copy(
            src_ref=src, dst_ref=dst, send_sem=send, recv_sem=recv,
            device_id={axis: peer}, device_id_type=MESH,
        )

    def part_copy(s, q, k):
        peer = partner(me, k, n)
        return remote(
            part.at[s, q, peer], slab.at[s, q, k], part_send.at[s, q, k], part_recv.at[s, q, k],
            "ra", peer,
        )

    def hid_copy(s, q, k, owner, peer):
        block = hslab.at[s, q, owner]
        return remote(block, block, hid_send.at[s, q, k], hid_recv.at[s, q, k], "ra", peer)

    def br_copy(s, q, k, owner, peer):
        block = bslab.at[s, q, owner]
        return remote(block, block, br_send.at[s, q, k], br_recv.at[s, q, k], "cb", peer)

    def project(s, q, v):
        square = jnp.sum(v * v, axis=1, keepdims=True)
        high = square.astype(BF16).astype(F32)
        low = square - high
        scaled = (v * gains[s]).astype(BF16)
        if s == 0 and q == 0:
            cast(0, 0)
            cast(0, 1)
        gate = dot_t(scaled, wg_h[s])
        up = dot_t(scaled, wu_h[s])
        for j in range(n):
            own = slice(j * t, (j + 1) * t)
            part[s, q, j, :, :f] = jnp.concatenate([gate[own], up[own]], axis=0).astype(BF16)
            part[s, q, j, :, f:] = jnp.broadcast_to(
                jnp.concatenate([high[own], low[own]], axis=0), (2 * t, width - f)
            ).astype(BF16)
        if s == 0 and q == 0:
            pl.semaphore_wait(barrier, n - 1 + m - 1)
        for k in far:
            part_copy(s, q, k).start()

    def activate(s, q):
        total = part[s, q, me].astype(F32)
        for k in far:
            part_copy(s, q, k).wait_recv()
            total = total + slab[s, q, k].astype(F32)
        square_total = total[:t, f : f + 1] + total[t:, f : f + 1]
        row_scale = lax.rsqrt(square_total / (d * n) + epsilon)
        gate_sum = total[:t, :f] * row_scale
        up_sum = total[t:, :f] * row_scale
        hslab[s, q, me] = (gate_sum / (1.0 + jnp.exp(-gate_sum)) * up_sum).astype(BF16)
        for k in far:
            hid_copy(s, q, k, me, partner(me, k, n)).start()

    def contract(s, q):
        for k in far:
            i = giver(me, k, n)
            hid_copy(s, q, k, i, i).wait_recv()
        hidden = jnp.concatenate([hslab[s, q, i].astype(F32) for i in range(n)], axis=0)
        branch_part = jnp.dot(hidden.astype(BF16), wd_h[s], preferred_element_type=F32)
        bslab[s, q, mc] = branch_part.astype(BF16)
        for k in wide:
            br_copy(s, q, k, mc, partner(mc, k, m)).start()

    def finish(s, q, v):
        for k in wide:
            i = giver(mc, k, m)
            br_copy(s, q, k, i, i).wait_recv()
        branch = bslab[s, q, 0].astype(F32)
        for i in range(1, m):
            branch = branch + bslab[s, q, i].astype(F32)
        return (residual_weight * v + branch).astype(BF16)

    for copy in small:
        copy.wait()
    streams = [x_ref[q * rows : (q + 1) * rows].astype(F32) for q in range(chains)]
    for q in range(chains):
        project(0, q, streams[q])
    cast(0, 2)
    for j in range(3):
        cast(1, j)
    for s in range(2):
        for q in range(chains):
            activate(s, q)
        for q in range(chains):
            contract(s, q)
        for q in range(chains):
            done = finish(s, q, streams[q])
            if s == 0:
                streams[q] = done.astype(F32)
                project(1, q, streams[q])
            else:
                out_ref[q * rows : (q + 1) * rows] = done

    for s in range(2):
        for q in range(chains):
            for k in far:
                part_copy(s, q, k).wait_send()
                hid_copy(s, q, k, me, partner(me, k, n)).wait_send()
            for k in wide:
                br_copy(s, q, k, mc, partner(mc, k, m)).wait_send()


def solution(mesh):
    n, m = mesh.shape["ra"], mesh.shape["cb"]

    def per_device(tokens, ga, wg_a, wu_a, wd_a, gb, wg_b, wu_b, wd_b):
        rows, d = tokens.shape
        f = wg_a.shape[1]
        chains = CHAINS if rows % (CHAINS * n) == 0 else 1
        t = rows // (n * chains)
        width = (f // 128 + 1) * 128
        vmem = pl.BlockSpec(memory_space=pltpu.VMEM)
        hbm = pl.BlockSpec(memory_space=pltpu.HBM)
        dma = pltpu.SemaphoreType.DMA
        return pl.pallas_call(
            functools.partial(kernel, n, m, chains),
            out_shape=jax.ShapeDtypeStruct((rows, d), BF16),
            in_specs=[hbm] * 9,
            out_specs=vmem,
            scratch_shapes=[
                pltpu.VMEM((rows, d), BF16),
                pltpu.VMEM((2, 1, d), F32),
                pltpu.VMEM((2, f, d), F32),
                pltpu.VMEM((2, f, d), F32),
                pltpu.VMEM((2, f, d), F32),
                pltpu.VMEM((2, f, d), BF16),
                pltpu.VMEM((2, f, d), BF16),
                pltpu.VMEM((2, f, d), BF16),
                pltpu.VMEM((2, chains, n, 2 * t, width), BF16),
                pltpu.VMEM((2, chains, n, 2 * t, width), BF16),
                pltpu.VMEM((2, chains, n, t, f), BF16),
                pltpu.VMEM((2, chains, m, rows // chains, d), BF16),
                dma((2, 3)), dma((3,)),
                dma((2, chains, n)), dma((2, chains, n)), dma((2, chains, n)),
                dma((2, chains, n)), dma((2, chains, m)), dma((2, chains, m)),
            ],
            compiler_params=pltpu.CompilerParams(collective_id=0, has_side_effects=True),
        )(tokens, ga.reshape(1, d), gb.reshape(1, d), wg_a.T, wu_a.T, wd_a, wg_b.T, wu_b.T, wd_b)

    weights = (P("ra", "cb"), P("ra", "cb"), P("cb", "ra"))
    placed = (P(None, "ra"), P("ra")) + weights + (P("ra"),) + weights
    return jax.shard_map(
        per_device, mesh=mesh, in_specs=placed, out_specs=P(None, "ra"), check_vma=False
    )
```

```python
import functools

import jax
import jax.numpy as jnp
from jax import lax
from jax.experimental import pallas as pl
from jax.experimental.pallas import tpu as pltpu
from jax.sharding import PartitionSpec as P

residual_weight = 0.5
epsilon = 1e-06
CHAINS = 1
VMEM_LIMIT = 56518246
MESH = pl.DeviceIdType.MESH
F32, BF16 = jnp.float32, jnp.bfloat16


def dot_t(a, b):
    return lax.dot_general(a, b, (((1,), (1,)), ((), ())), preferred_element_type=F32)


def partner(me, k, n):
    if n & (n - 1):
        return lax.rem(me + k, n)
    peer, bit = me, 1
    while bit < n:
        if k & bit:
            peer = peer + bit - 2 * bit * ((me // bit) % 2)
        bit *= 2
    return peer


def send_order(n):
    if n % 2:
        return list(range(n - 1, 0, -1))
    pairs = sorted(range(1, n // 2), key=lambda z: (abs(z - n // 4), -z))
    return [2 * z + 1 for z in pairs] + [2 * z for z in pairs] + [1]


def giver(me, k, n):
    return lax.rem(me + n - k, n) if n & (n - 1) else partner(me, k, n)


def kernel(
    n, m, chains, x_in, gain_a, gain_b, wg_a, wu_a, wd_a, wg_b, wu_b, wd_b, out_ref,
    x_ref, gains, wg_f, wu_f, wd_f, wg_h, wu_h, wd_h, part, slab, hslab, bslab,
    load_sem, small_sem, part_send, part_recv, hid_send, hid_recv, br_send, br_recv,
):
    me = lax.axis_index("ra")
    mc = lax.axis_index("cb")
    tokens, d = x_in.shape
    f = wg_a.shape[0]
    rows = tokens // chains
    t = rows // n
    width = part.shape[-1]
    far = send_order(n)
    wide = range(m - 1, 0, -1)

    barrier = pltpu.get_barrier_semaphore()
    for k in far:
        pl.semaphore_signal(
            barrier, inc=1, device_id={"ra": partner(me, k, n)}, device_id_type=MESH
        )
    for k in wide:
        pl.semaphore_signal(
            barrier, inc=1, device_id={"cb": partner(mc, k, m)}, device_id_type=MESH
        )

    small = [
        pltpu.make_async_copy(x_in, x_ref, small_sem.at[0]),
        pltpu.make_async_copy(gain_a, gains.at[0], small_sem.at[1]),
        pltpu.make_async_copy(gain_b, gains.at[1], small_sem.at[2]),
    ]
    for copy in small:
        copy.start()
    loads = {}
    for s, (g, u, w) in enumerate(((wg_a, wu_a, wd_a), (wg_b, wu_b, wd_b))):
        for j, (src, dst) in enumerate(((g, wg_f), (u, wu_f), (w, wd_f))):
            loads[s, j] = pltpu.make_async_copy(src, dst.at[s], load_sem.at[s, j])
            loads[s, j].start()

    def cast(s, j):
        src, dst = ((wg_f, wg_h), (wu_f, wu_h), (wd_f, wd_h))[j]
        loads[s, j].wait()
        dst[s] = src[s].astype(BF16)

    def remote(src, dst, send, recv, axis, peer):
        return pltpu.make_async_remote_copy(
            src_ref=src, dst_ref=dst, send_sem=send, recv_sem=recv,
            device_id={axis: peer}, device_id_type=MESH,
        )

    def part_copy(s, q, k):
        peer = partner(me, k, n)
        return remote(
            part.at[s, q, peer], slab.at[s, q, k], part_send.at[s, q, k], part_recv.at[s, q, k],
            "ra", peer,
        )

    def hid_copy(s, q, k, owner, peer):
        block = hslab.at[s, q, owner]
        return remote(block, block, hid_send.at[s, q, k], hid_recv.at[s, q, k], "ra", peer)

    def br_copy(s, q, k, owner, peer):
        block = bslab.at[s, q, owner]
        return remote(block, block, br_send.at[s, q, k], br_recv.at[s, q, k], "cb", peer)

    def project(s, q, v):
        square = jnp.sum(v * v, axis=1, keepdims=True)
        high = square.astype(BF16).astype(F32)
        low = square - high
        scaled = (v * gains[s]).astype(BF16)
        if s == 0 and q == 0:
            cast(0, 0)
            cast(0, 1)
        gate = dot_t(scaled, wg_h[s])
        up = dot_t(scaled, wu_h[s])
        for j in range(n):
            own = slice(j * t, (j + 1) * t)
            part[s, q, j, :, :f] = jnp.concatenate([gate[own], up[own]], axis=0).astype(BF16)
            part[s, q, j, :, f:] = jnp.broadcast_to(
                jnp.concatenate([high[own], low[own]], axis=0), (2 * t, width - f)
            ).astype(BF16)
        if s == 0 and q == 0:
            pl.semaphore_wait(barrier, n - 1 + m - 1)
        for k in far:
            part_copy(s, q, k).start()

    def activate(s, q):
        total = part[s, q, me].astype(F32)
        for k in far:
            part_copy(s, q, k).wait_recv()
            total = total + slab[s, q, k].astype(F32)
        square_total = total[:t, f : f + 1] + total[t:, f : f + 1]
        row_scale = lax.rsqrt(square_total / (d * n) + epsilon)
        gate_sum = total[:t, :f] * row_scale
        up_sum = total[t:, :f] * row_scale
        hslab[s, q, me] = (gate_sum / (1.0 + jnp.exp(-gate_sum)) * up_sum).astype(BF16)
        for k in far:
            hid_copy(s, q, k, me, partner(me, k, n)).start()

    def contract(s, q):
        for k in far:
            i = giver(me, k, n)
            hid_copy(s, q, k, i, i).wait_recv()
        hidden = jnp.concatenate([hslab[s, q, i].astype(F32) for i in range(n)], axis=0)
        branch_part = jnp.dot(hidden.astype(BF16), wd_h[s], preferred_element_type=F32)
        bslab[s, q, mc] = branch_part.astype(BF16)
        for k in wide:
            br_copy(s, q, k, mc, partner(mc, k, m)).start()

    def finish(s, q, v):
        for k in wide:
            i = giver(mc, k, m)
            br_copy(s, q, k, i, i).wait_recv()
        branch = bslab[s, q, 0].astype(F32)
        for i in range(1, m):
            branch = branch + bslab[s, q, i].astype(F32)
        return (residual_weight * v + branch).astype(BF16)

    for copy in small:
        copy.wait()
    streams = [x_ref[q * rows : (q + 1) * rows].astype(F32) for q in range(chains)]
    for q in range(chains):
        project(0, q, streams[q])
    cast(0, 2)
    for j in range(3):
        cast(1, j)
    for s in range(2):
        for q in range(chains):
            activate(s, q)
        for q in range(chains):
            contract(s, q)
        for q in range(chains):
            done = finish(s, q, streams[q])
            if s == 0:
                streams[q] = done.astype(F32)
                project(1, q, streams[q])
            else:
                out_ref[q * rows : (q + 1) * rows] = done

    for s in range(2):
        for q in range(chains):
            for k in far:
                part_copy(s, q, k).wait_send()
                hid_copy(s, q, k, me, partner(me, k, n)).wait_send()
            for k in wide:
                br_copy(s, q, k, mc, partner(mc, k, m)).wait_send()


def solution(mesh):
    n, m = mesh.shape["ra"], mesh.shape["cb"]

    def per_device(tokens, ga, wg_a, wu_a, wd_a, gb, wg_b, wu_b, wd_b):
        rows, d = tokens.shape
        f = wg_a.shape[1]
        chains = CHAINS if rows % (CHAINS * n) == 0 else 1
        t = rows // (n * chains)
        width = (f // 128 + 1) * 128
        vmem = pl.BlockSpec(memory_space=pltpu.VMEM)
        hbm = pl.BlockSpec(memory_space=pltpu.HBM)
        dma = pltpu.SemaphoreType.DMA
        return pl.pallas_call(
            functools.partial(kernel, n, m, chains),
            out_shape=jax.ShapeDtypeStruct((rows, d), BF16),
            in_specs=[hbm] * 9,
            out_specs=vmem,
            scratch_shapes=[
                pltpu.VMEM((rows, d), BF16),
                pltpu.VMEM((2, 1, d), F32),
                pltpu.VMEM((2, f, d), F32),
                pltpu.VMEM((2, f, d), F32),
                pltpu.VMEM((2, f, d), F32),
                pltpu.VMEM((2, f, d), BF16),
                pltpu.VMEM((2, f, d), BF16),
                pltpu.VMEM((2, f, d), BF16),
                pltpu.VMEM((2, chains, n, 2 * t, width), BF16),
                pltpu.VMEM((2, chains, n, 2 * t, width), BF16),
                pltpu.VMEM((2, chains, n, t, f), BF16),
                pltpu.VMEM((2, chains, m, rows // chains, d), BF16),
                dma((2, 3)), dma((3,)),
                dma((2, chains, n)), dma((2, chains, n)), dma((2, chains, n)),
                dma((2, chains, n)), dma((2, chains, m)), dma((2, chains, m)),
            ],
            compiler_params=pltpu.CompilerParams(collective_id=0, has_side_effects=True, vmem_limit_bytes=VMEM_LIMIT),
        )(tokens, ga.reshape(1, d), gb.reshape(1, d), wg_a.T, wu_a.T, wd_a, wg_b.T, wu_b.T, wd_b)

    weights = (P("ra", "cb"), P("ra", "cb"), P("cb", "ra"))
    placed = (P(None, "ra"), P("ra")) + weights + (P("ra"),) + weights
    return jax.shard_map(
        per_device, mesh=mesh, in_specs=placed, out_specs=P(None, "ra"), check_vma=False
    )
```

```python
import functools

import jax
import jax.numpy as jnp
from jax import lax
from jax.experimental import pallas as pl
from jax.experimental.pallas import tpu as pltpu
from jax.sharding import PartitionSpec as P

residual_weight = 0.5
epsilon = 1e-06
CHAINS = 1
VMEM_LIMIT = 56518246
MESH = pl.DeviceIdType.MESH
F32, BF16 = jnp.float32, jnp.bfloat16


def dot_t(a, b):
    return lax.dot_general(a, b, (((1,), (1,)), ((), ())), preferred_element_type=F32)


def partner(me, k, n):
    if n & (n - 1):
        return lax.rem(me + k, n)
    peer, bit = me, 1
    while bit < n:
        if k & bit:
            peer = peer + bit - 2 * bit * ((me // bit) % 2)
        bit *= 2
    return peer


def send_order(n):
    if n % 2:
        return list(range(n - 1, 0, -1))
    pairs = sorted(range(1, n // 2), key=lambda z: (abs(z - n // 4), -z))
    return [2 * z + 1 for z in pairs] + [2 * z for z in pairs] + [1]


def giver(me, k, n):
    return lax.rem(me + n - k, n) if n & (n - 1) else partner(me, k, n)


def kernel(
    n, m, chains, x_in, gain_a, gain_b, wg_a, wu_a, wd_a, wg_b, wu_b, wd_b, out_ref,
    x_ref, gains, wg_f, wu_f, wd_f, wg_h, wu_h, wd_h, part, slab, hslab, bslab,
    load_sem, small_sem, part_send, part_recv, hid_send, hid_recv, br_send, br_recv,
):
    me = lax.axis_index("ra")
    mc = lax.axis_index("cb")
    tokens, d = x_in.shape
    f = wg_a.shape[0]
    rows = tokens // chains
    t = rows // n
    width = part.shape[-1]
    far = send_order(n)
    wide = range(m - 1, 0, -1)

    barrier = pltpu.get_barrier_semaphore()
    for k in far:
        pl.semaphore_signal(
            barrier, inc=1, device_id={"ra": partner(me, k, n)}, device_id_type=MESH
        )
    for k in wide:
        pl.semaphore_signal(
            barrier, inc=1, device_id={"cb": partner(mc, k, m)}, device_id_type=MESH
        )

    small = [
        pltpu.make_async_copy(x_in, x_ref, small_sem.at[0]),
        pltpu.make_async_copy(gain_a, gains.at[0], small_sem.at[1]),
        pltpu.make_async_copy(gain_b, gains.at[1], small_sem.at[2]),
    ]
    for copy in small:
        copy.start()
    loads = {}
    for s, (g, u, w) in enumerate(((wg_a, wu_a, wd_a), (wg_b, wu_b, wd_b))):
        for j, (src, dst) in enumerate(((g, wg_f), (u, wu_f), (w, wd_f))):
            loads[s, j] = pltpu.make_async_copy(src, dst.at[s], load_sem.at[s, j])
            loads[s, j].start()

    def cast(s, j):
        src, dst = ((wg_f, wg_h), (wu_f, wu_h), (wd_f, wd_h))[j]
        loads[s, j].wait()
        dst[s] = src[s].astype(BF16)

    def remote(src, dst, send, recv, axis, peer):
        return pltpu.make_async_remote_copy(
            src_ref=src, dst_ref=dst, send_sem=send, recv_sem=recv,
            device_id={axis: peer}, device_id_type=MESH,
        )

    def part_copy(s, q, k):
        peer = partner(me, k, n)
        return remote(
            part.at[s, q, peer], slab.at[s, q, k], part_send.at[s, q, k], part_recv.at[s, q, k],
            "ra", peer,
        )

    def hid_copy(s, q, k, owner, peer):
        block = hslab.at[s, q, owner]
        return remote(block, block, hid_send.at[s, q, k], hid_recv.at[s, q, k], "ra", peer)

    def br_copy(s, q, k, owner, peer):
        block = bslab.at[s, q, owner]
        return remote(block, block, br_send.at[s, q, k], br_recv.at[s, q, k], "cb", peer)

    def project(s, q, v):
        square = jnp.sum(v * v, axis=1, keepdims=True)
        high = square.astype(BF16).astype(F32)
        low = square - high
        scaled = (v * gains[s]).astype(BF16)
        if s == 0 and q == 0:
            cast(0, 0)
            cast(0, 1)
        gate = dot_t(scaled, wg_h[s])
        up = dot_t(scaled, wu_h[s])
        for j in range(n):
            own = slice(j * t, (j + 1) * t)
            part[s, q, j, :, :f] = jnp.concatenate([gate[own], up[own]], axis=0).astype(BF16)
            part[s, q, j, :, f:] = jnp.broadcast_to(
                jnp.concatenate([high[own], low[own]], axis=0), (2 * t, width - f)
            ).astype(BF16)
        if s == 0 and q == 0:
            pl.semaphore_wait(barrier, n - 1 + m - 1)
        for k in far:
            part_copy(s, q, k).start()

    def activate(s, q):
        total = part[s, q, me].astype(F32)
        for k in far:
            part_copy(s, q, k).wait_recv()
            total = total + slab[s, q, k].astype(F32)
        square_total = total[:t, f : f + 1] + total[t:, f : f + 1]
        row_scale = lax.rsqrt(square_total / (d * n) + epsilon)
        gate_sum = total[:t, :f] * row_scale
        up_sum = total[t:, :f] * row_scale
        hslab[s, q, me] = (gate_sum / (1.0 + jnp.exp(-gate_sum)) * up_sum).astype(BF16)
        for k in far:
            hid_copy(s, q, k, me, partner(me, k, n)).start()

    def contract(s, q):
        for k in far:
            i = giver(me, k, n)
            hid_copy(s, q, k, i, i).wait_recv()
        hidden = jnp.concatenate([hslab[s, q, i] for i in range(n)], axis=0)
        branch_part = jnp.dot(hidden, wd_h[s], preferred_element_type=F32)
        bslab[s, q, mc] = branch_part.astype(BF16)
        for k in wide:
            br_copy(s, q, k, mc, partner(mc, k, m)).start()

    def finish(s, q, v):
        for k in wide:
            i = giver(mc, k, m)
            br_copy(s, q, k, i, i).wait_recv()
        branch = bslab[s, q, 0].astype(F32)
        for i in range(1, m):
            branch = branch + bslab[s, q, i].astype(F32)
        return (residual_weight * v + branch).astype(BF16)

    for copy in small:
        copy.wait()
    streams = [x_ref[q * rows : (q + 1) * rows].astype(F32) for q in range(chains)]
    for q in range(chains):
        project(0, q, streams[q])
    cast(0, 2)
    for j in range(3):
        cast(1, j)
    for s in range(2):
        for q in range(chains):
            activate(s, q)
        for q in range(chains):
            contract(s, q)
        for q in range(chains):
            done = finish(s, q, streams[q])
            if s == 0:
                streams[q] = done.astype(F32)
                project(1, q, streams[q])
            else:
                out_ref[q * rows : (q + 1) * rows] = done

    for s in range(2):
        for q in range(chains):
            for k in far:
                part_copy(s, q, k).wait_send()
                hid_copy(s, q, k, me, partner(me, k, n)).wait_send()
            for k in wide:
                br_copy(s, q, k, mc, partner(mc, k, m)).wait_send()


def solution(mesh):
    n, m = mesh.shape["ra"], mesh.shape["cb"]

    def per_device(tokens, ga, wg_a, wu_a, wd_a, gb, wg_b, wu_b, wd_b):
        rows, d = tokens.shape
        f = wg_a.shape[1]
        chains = CHAINS if rows % (CHAINS * n) == 0 else 1
        t = rows // (n * chains)
        width = (f // 128 + 1) * 128
        vmem = pl.BlockSpec(memory_space=pltpu.VMEM)
        hbm = pl.BlockSpec(memory_space=pltpu.HBM)
        dma = pltpu.SemaphoreType.DMA
        return pl.pallas_call(
            functools.partial(kernel, n, m, chains),
            out_shape=jax.ShapeDtypeStruct((rows, d), BF16),
            in_specs=[hbm] * 9,
            out_specs=vmem,
            scratch_shapes=[
                pltpu.VMEM((rows, d), BF16),
                pltpu.VMEM((2, 1, d), F32),
                pltpu.VMEM((2, f, d), F32),
                pltpu.VMEM((2, f, d), F32),
                pltpu.VMEM((2, f, d), F32),
                pltpu.VMEM((2, f, d), BF16),
                pltpu.VMEM((2, f, d), BF16),
                pltpu.VMEM((2, f, d), BF16),
                pltpu.VMEM((2, chains, n, 2 * t, width), BF16),
                pltpu.VMEM((2, chains, n, 2 * t, width), BF16),
                pltpu.VMEM((2, chains, n, t, f), BF16),
                pltpu.VMEM((2, chains, m, rows // chains, d), BF16),
                dma((2, 3)), dma((3,)),
                dma((2, chains, n)), dma((2, chains, n)), dma((2, chains, n)),
                dma((2, chains, n)), dma((2, chains, m)), dma((2, chains, m)),
            ],
            compiler_params=pltpu.CompilerParams(collective_id=0, has_side_effects=True, vmem_limit_bytes=VMEM_LIMIT),
        )(tokens, ga.reshape(1, d), gb.reshape(1, d), wg_a.T, wu_a.T, wd_a, wg_b.T, wu_b.T, wd_b)

    weights = (P("ra", "cb"), P("ra", "cb"), P("cb", "ra"))
    placed = (P(None, "ra"), P("ra")) + weights + (P("ra"),) + weights
    return jax.shard_map(
        per_device, mesh=mesh, in_specs=placed, out_specs=P(None, "ra"), check_vma=False
    )
```
